32 devices in a mesh: ep: 8 (over z, x), tp: 4 (over y, core).
Axes of the slice: x: 2, y: 2, z: 4, core: 2. Of those that a mesh axis runs over, the one named last changes fastest.
Arguments:
- mix_query: bfloat16 [16384, 2048], P('ep', 'tp'), may hold values from -6 to 6
- mix_key: bfloat16 [16384, 2048], P('ep', 'tp'), may hold values from -6 to 6
- mix_value: bfloat16 [16384, 2048], P('ep', 'tp'), may hold values from -6 to 6
- mix_gate: bfloat16 [16384, 2048], P('ep', 'tp'), may hold values from -6 to 6
- log_decay: float32 [16384, 8], P('ep', 'tp'), may hold values from -1 to 0, as said below
- ret_gain: float32 [2048], P('tp'), may hold values from 0.1 to 1.9
- w_out: bfloat16 [2048, 2048], replicated, may hold values from -0.125 to 0.125
- moe_in: bfloat16 [1024, 2048], P(('ep', 'tp')), may hold values from -6 to 6
- route_ids: int32 [1024, 2], P(('ep', 'tp')), may hold values from 0 to 7, as said below
- route_weights: float32 [1024, 2], P(('ep', 'tp')), may hold values from 0.1 to 1
- moe_gain: float32 [2048], replicated, may hold values from 0.1 to 1.9
- w_gate: bfloat16 [8, 2048, 7168], P('ep', None, 'tp'), may hold values from -0.125 to 0.125
- w_up: bfloat16 [8, 2048, 7168], P('ep', None, 'tp'), may hold values from -0.125 to 0.125
- w_down: bfloat16 [8, 7168, 2048], P('ep', 'tp'), may hold values from -0.0625 to 0.0625
Outputs:
- mix_out: bfloat16 [16384, 2048], P(('ep', 'tp'))
- moe_out: bfloat16 [1024, 2048], P(('ep', 'tp'))
The draws below stay inside these ranges and needn't reach their ends.
Inputs may be any that keep to these rules, and one draw needn't show every extreme that they name: `log_decay`: log of a decay. `route_ids`: each row names 2 different experts. Among the rows of one device no expert is named by more than 16 rows, and one expert is named by exactly 16 rows of every device.
All inputs are finite; a program needn't handle non-finite values.
Results may differ from the reference program's by a relative error of at most 0.015.
Values may be sent and summed in bfloat16 or wider, within the bound.
A program may use at most 128 MiB of HBM per device.

```python
import math
import jax
import jax.numpy as jnp
from jax import lax

D = 2048
FF = 7168
RETENTION_HEADS = 8
HEAD_DIM = 256
BLOCK = 512
TOP = 2
SEQ_DEV = 2048
MOE_DEV = 32
SEQUENCE_LENGTH = 16384
MOE_TOK = 1024
EXPERTS = 8
CAP = 16
N_TP = 4


def block_permutation(perm_key, length):
    return jax.random.permutation(perm_key, length)


def draw_route_ids(key, part):
    block_count = MOE_TOK // MOE_DEV
    half_cap = CAP // 2
    pair_count = (EXPERTS - 2) // 2
    base_key = jax.random.fold_in(key, 31)
    key_star, key_order, key_delta, key_shuffle = jax.random.split(base_key, 4)
    star = jax.random.randint(key_star, (), 0, EXPERTS)
    others = (star + 1 + jnp.arange(EXPERTS - 1, dtype=jnp.int32)) % EXPERTS
    order_keys = jax.random.split(key_order, block_count)
    orders = jax.vmap(block_permutation, in_axes=(0, None))(order_keys, EXPERTS - 1)
    ranked = others[orders]
    delta = jax.random.randint(key_delta, (block_count, pair_count), 0, half_cap + 1)
    pair_counts = jnp.stack([half_cap + delta, half_cap - delta], axis=-1).reshape(block_count, 2 * pair_count)
    counts = jnp.concatenate([jnp.full((block_count, 1), CAP, jnp.int32), pair_counts.astype(jnp.int32), jnp.zeros((block_count, 1), jnp.int32)], axis=1)
    listed = jnp.concatenate([jnp.full((block_count, 1), star, jnp.int32), ranked.astype(jnp.int32)], axis=1)
    bounds = jnp.cumsum(counts, axis=1)
    slots = jnp.arange(2 * MOE_DEV, dtype=jnp.int32)
    position = jnp.sum((slots[None, :, None] >= bounds[:, None, :]).astype(jnp.int32), axis=-1)
    chosen = jnp.take_along_axis(listed, position, axis=1)
    paired = jnp.stack([chosen[:, :MOE_DEV], chosen[:, MOE_DEV:]], axis=-1)
    shuffle_keys = jax.random.split(key_shuffle, block_count)
    shuffles = jax.vmap(block_permutation, in_axes=(0, None))(shuffle_keys, MOE_DEV)
    paired = jnp.take_along_axis(paired, shuffles[:, :, None], axis=1)
    return paired.reshape(MOE_TOK, TOP).astype(jnp.int32)


def draw_log_decay(key, part):
    base_key = jax.random.fold_in(key, 53)
    random_keys = jax.random.split(base_key, 6)
    fast_heads = jax.random.uniform(random_keys[0], (RETENTION_HEADS,)) < 0.5
    fast_rate = 1.0 / jax.random.uniform(random_keys[1], (RETENTION_HEADS,), minval=30.0, maxval=100.0)
    slow_rate = jax.random.uniform(random_keys[2], (RETENTION_HEADS,), minval=0.05, maxval=0.2) * math.log(10.0) / SEQUENCE_LENGTH
    per_head_decay = jnp.where(fast_heads, fast_rate, slow_rate)
    device_factor = jnp.exp(jax.random.uniform(random_keys[3], (SEQUENCE_LENGTH // SEQ_DEV,), minval=math.log(0.5), maxval=math.log(2.0)))
    position_index = jnp.arange(SEQUENCE_LENGTH, dtype=jnp.int32)
    decay_factor_lookup = device_factor[position_index // SEQ_DEV]
    spike_position = jax.random.randint(random_keys[4], (RETENTION_HEADS, 2), 0, SEQUENCE_LENGTH)
    spike_length = jnp.log(jax.random.uniform(random_keys[5], (RETENTION_HEADS, 2), minval=0.5, maxval=0.8))
    spike_matches = position_index[:, None, None] == spike_position[None, :, :]
    spike_list = jnp.sum(jnp.where(spike_matches, spike_length[None, :, :], 0.0), axis=-1)
    return (-per_head_decay[None, :] * decay_factor_lookup[:, None] + spike_list).astype(jnp.float32)


def steps_of(rng, dims, shards, smallest, high):
    def one(axis_at, shards_of):
        draws = jax.random.uniform(jax.random.fold_in(jax.random.fold_in(rng, 6), axis_at), (shards_of,), jnp.float32, smallest / len(shards), high / len(shards))
        return jnp.repeat(jnp.exp(draws), dims[axis_at] // shards_of).reshape((-1,) + (1,) * (len(dims) - axis_at - 1))

    gain = one(*shards[0])
    for cut in shards[1:]:
        gain = gain * one(*cut)
    return gain


def noise(rng, dims, width, most, cuts=(), kind=jnp.bfloat16):
    drawn = width * jax.random.normal(rng, dims, jnp.float32)
    if cuts:
        drawn = drawn * steps_of(rng, dims, cuts, -0.22, 0.18)
    return jnp.clip(drawn, -most, most).astype(kind)


def setup_inputs(seed: int = 0) -> dict:
    splits = jax.random.split(jax.random.key(seed), 15)
    mix_query = noise(splits[0], (SEQUENCE_LENGTH, RETENTION_HEADS * HEAD_DIM), 1.0, 6.0, ((0, 8), (1, 4)))
    mix_key = noise(splits[1], (SEQUENCE_LENGTH, RETENTION_HEADS * HEAD_DIM), 1.0, 6.0, ((0, 8), (1, 4)))
    mix_value = noise(splits[2], (SEQUENCE_LENGTH, RETENTION_HEADS * HEAD_DIM), 1.0, 6.0, ((0, 8), (1, 4)))
    mix_gate = noise(splits[3], (SEQUENCE_LENGTH, RETENTION_HEADS * HEAD_DIM), 1.0, 6.0, ((0, 8), (1, 4)))
    log_decay = draw_log_decay(jax.random.fold_in(splits[14], 71), 0)
    ret_gain = jnp.clip(1.0 + 0.18 * jax.random.normal(splits[5], (RETENTION_HEADS * HEAD_DIM,), jnp.float32), 0.1, 1.9)
    w_out = noise(splits[6], (RETENTION_HEADS * HEAD_DIM, D), (RETENTION_HEADS * HEAD_DIM) ** -0.5, 0.125)
    moe_in = noise(splits[7], (MOE_TOK, D), 1.0, 6.0, ((0, 32),))
    route_ids = draw_route_ids(jax.random.fold_in(splits[14], 71), 0)
    route_weights = jnp.clip(0.1 + 0.9 * jax.random.uniform(splits[9], (MOE_TOK, TOP), jnp.float32) ** steps_of(splits[9], (MOE_TOK, TOP), ((0, 32),), -0.2, 0.2), 0.1, 1.0)
    moe_gain = jnp.clip(1.0 + 0.18 * jax.random.normal(splits[10], (D,), jnp.float32), 0.1, 1.9)
    w_gate = noise(splits[11], (EXPERTS, D, FF), D ** -0.5, 0.125, ((0, 8), (2, 4)))
    w_up = noise(splits[12], (EXPERTS, D, FF), D ** -0.5, 0.125, ((0, 8), (2, 4)))
    w_down = noise(splits[13], (EXPERTS, FF, D), FF ** -0.5, 0.0625, ((0, 8), (1, 4)))
    return dict(mix_query=mix_query, mix_key=mix_key, mix_value=mix_value, mix_gate=mix_gate, log_decay=log_decay, ret_gain=ret_gain, w_out=w_out, moe_in=moe_in, route_ids=route_ids, route_weights=route_weights, moe_gain=moe_gain, w_gate=w_gate, w_up=w_up, w_down=w_down)


norm_eps = 1e-06

def rotate(tensor, position_index):
    head_dim = tensor.shape[-1]
    half_dim = head_dim // 2
    inverse = 10000.0 ** (-(jnp.arange(half_dim, dtype=jnp.float32) * 2.0) / head_dim)
    angle = position_index.astype(jnp.float32)[:, None] * inverse[None, :]
    cosine = jnp.cos(angle)[:, None, :]
    sine = jnp.sin(angle)[:, None, :]
    front = tensor[..., :half_dim]
    back = tensor[..., half_dim:]
    return jnp.concatenate([front * cosine - back * sine, back * cosine + front * sine], axis=-1)

def retention_blocks(query_rot, key_rot, values, log_decay):
    length = query_rot.shape[0]
    block_count = length // BLOCK
    query_blocks = query_rot.reshape(block_count, BLOCK, RETENTION_HEADS, HEAD_DIM)
    key_blocks = key_rot.reshape(block_count, BLOCK, RETENTION_HEADS, HEAD_DIM)
    value_blocks = values.reshape(block_count, BLOCK, RETENTION_HEADS, HEAD_DIM)
    cumulative = jnp.cumsum(log_decay.reshape(block_count, BLOCK, RETENTION_HEADS), axis=1)
    causal = jnp.arange(BLOCK)[:, None] >= jnp.arange(BLOCK)[None, :]

    def advance(carried, block_items):
        query_now, key_now, value_now, cumul_now = block_items
        scores = jnp.einsum('ihd,jhd->hij', query_now.astype(jnp.float32), key_now.astype(jnp.float32))
        by_head = cumul_now.T
        log_gap = by_head[:, :, None] - by_head[:, None, :]
        decay_mask = jnp.where(causal[None], jnp.exp(jnp.where(causal[None], log_gap, 0.0)), 0.0)
        weights = (scores * decay_mask).astype(jnp.bfloat16)
        within_block = jnp.einsum('hij,jhe->ihe', weights.astype(jnp.float32), value_now.astype(jnp.float32))
        block_last = cumul_now[-1]
        query_decayed = query_now.astype(jnp.float32) * jnp.exp(cumul_now)[:, :, None]
        carried_part = jnp.einsum('ihd,hde->ihe', query_decayed, carried, precision=lax.Precision.HIGHEST)
        key_decayed = (key_now.astype(jnp.float32) * jnp.exp(block_last[None, :] - cumul_now)[:, :, None]).astype(jnp.bfloat16)
        update = jnp.einsum('jhd,jhe->hde', key_decayed.astype(jnp.float32), value_now.astype(jnp.float32))
        return (jnp.exp(block_last)[:, None, None] * carried + update, within_block + carried_part)
    initial = jnp.zeros((RETENTION_HEADS, HEAD_DIM, HEAD_DIM), jnp.float32)
    final_state, outputs = lax.scan(advance, initial, (query_blocks, key_blocks, value_blocks, cumulative))
    return outputs.reshape(length, RETENTION_HEADS, HEAD_DIM)

def mixer_reference(mix_query, mix_key, mix_value, mix_gate, log_decay, ret_gain, w_out):
    length = mix_query.shape[0]
    position_index = jnp.arange(length, dtype=jnp.int32)
    query_rot = rotate(mix_query.astype(jnp.float32).reshape(length, RETENTION_HEADS, HEAD_DIM), position_index).astype(jnp.bfloat16)
    key_rot = (rotate(mix_key.astype(jnp.float32).reshape(length, RETENTION_HEADS, HEAD_DIM), position_index) * HEAD_DIM ** (-0.5)).astype(jnp.bfloat16)
    values = mix_value.reshape(length, RETENTION_HEADS, HEAD_DIM)
    retained = retention_blocks(query_rot, key_rot, values, log_decay)
    inverse_rms = lax.rsqrt(lax.optimization_barrier(jnp.mean(retained * retained, axis=-1, keepdims=True)) + norm_eps)
    gate_act = jax.nn.silu(mix_gate.astype(jnp.float32).reshape(length, RETENTION_HEADS, HEAD_DIM))
    heads_out = (gate_act * retained * inverse_rms * ret_gain.reshape(RETENTION_HEADS, HEAD_DIM)).astype(jnp.bfloat16)
    projected = jnp.dot(heads_out.reshape(length, RETENTION_HEADS * HEAD_DIM), w_out, preferred_element_type=jnp.float32)
    return projected.astype(jnp.bfloat16)

def expert_reference(moe_in, route_ids, route_weights, moe_gain, w_gate, w_up, w_down):
    tokens = moe_in.shape[0]
    model_width = moe_in.shape[1]
    block_count = tokens // MOE_DEV
    floats = moe_in.astype(jnp.float32)
    normed = (floats * lax.rsqrt(lax.optimization_barrier(jnp.mean(floats * floats, axis=-1, keepdims=True)) + norm_eps) * moe_gain).astype(jnp.bfloat16)
    block_ids = route_ids.reshape(block_count, MOE_DEV * TOP)
    onehot = (block_ids[:, :, None] == jnp.arange(EXPERTS, dtype=jnp.int32)[None, None, :]).astype(jnp.int32)
    slot_index = lax.optimization_barrier(jnp.sum(jnp.cumsum(onehot, axis=1) * onehot, axis=-1)) - 1
    buffer_rows = (jnp.arange(block_count, dtype=jnp.int32)[:, None] * CAP + slot_index).reshape(-1)
    token_index = (jnp.arange(block_count, dtype=jnp.int32)[:, None] * MOE_DEV + jnp.arange(MOE_DEV * TOP, dtype=jnp.int32)[None, :] // TOP).reshape(-1)
    flat_ids = block_ids.reshape(-1)
    buffer = jnp.zeros((EXPERTS, block_count * CAP, model_width), jnp.bfloat16)
    buffer = buffer.at[flat_ids, buffer_rows].set(normed[token_index])
    group_width = FF // N_TP

    def one_expert(expert_items):
        row_block, gate_weight, up_weight, down_weight = expert_items
        gate_part = jnp.dot(row_block, gate_weight, preferred_element_type=jnp.float32)
        up_part = jnp.dot(row_block, up_weight, preferred_element_type=jnp.float32)
        hidden = (jax.nn.silu(gate_part) * up_part).astype(jnp.bfloat16)
        summed = jnp.zeros((row_block.shape[0], model_width), jnp.float32)
        for group in range(N_TP):
            partial_value = jnp.dot(hidden[:, group * group_width:(group + 1) * group_width], down_weight[group * group_width:(group + 1) * group_width], preferred_element_type=jnp.float32).astype(jnp.bfloat16)
            summed = summed + partial_value.astype(jnp.float32)
        return summed.astype(jnp.bfloat16)
    outputs = lax.map(one_expert, (buffer, w_gate, w_up, w_down))
    picked = outputs[flat_ids, buffer_rows].reshape(tokens, TOP, model_width)
    combined = lax.optimization_barrier(jnp.sum(picked.astype(jnp.float32) * route_weights[:, :, None], axis=1))
    return combined.astype(jnp.bfloat16)

def reference(mix_query, mix_key, mix_value, mix_gate, log_decay, ret_gain, w_out, moe_in, route_ids, route_weights, moe_gain, w_gate, w_up, w_down):
    mix_out = mixer_reference(mix_query, mix_key, mix_value, mix_gate, log_decay, ret_gain, w_out)
    moe_out = expert_reference(moe_in, route_ids, route_weights, moe_gain, w_gate, w_up, w_down)
    return (mix_out, moe_out)
```

```python
import functools

import jax
import jax.numpy as jnp
import numpy as np
from jax import lax
from jax.experimental import pallas as pl
from jax.experimental.pallas import tpu as pltpu
from jax.sharding import PartitionSpec as P

HEAD_DIM = 256
BLOCK = 512
norm_eps = 1e-06
F32 = jnp.float32
BF16 = jnp.bfloat16
MESH = pl.DeviceIdType.MESH
VMEM_LIMIT = 67043328
COLS = 512


def dot(a, b, ca=1, cb=0):
    return lax.dot_general(a, b, (((ca,), (cb,)), ((), ())), preferred_element_type=F32)


def split3(x):
    a = x.astype(BF16)
    rest = x - a.astype(F32)
    b = rest.astype(BF16)
    c = (rest - b.astype(F32)).astype(BF16)
    return a, b, c


def loop(count, body):
    def step(i, carry):
        body(i)
        return carry

    lax.fori_loop(0, count, step, 0)


def slots_of(ids, capacity, count):
    tokens = ids.shape[1]
    row = lax.broadcasted_iota(jnp.int32, (count, tokens), 0)
    expert = row // capacity
    first = ids[0:1, :] == expert
    second = ids[1:2, :] == expert
    member = jnp.where(first | second, 1.0, 0.0)
    earlier = jnp.where(
        lax.broadcasted_iota(jnp.int32, (tokens, tokens), 0)
        < lax.broadcasted_iota(jnp.int32, (tokens, tokens), 1),
        1.0,
        0.0,
    ).astype(BF16)
    taken = dot(member.astype(BF16), earlier)
    slot = (row - expert * capacity).astype(F32)
    return jnp.where(taken == slot, member, 0.0), first


def layer_kernel(
    x_ref, ids_ref, rw_ref, mgain_ref, rgain_ref, logs_ref, cos_r, sin_r, cos_b, sin_b,
    q_hbm, k_hbm, v_hbm, g_hbm, wg_hbm, wu_hbm, wd_hbm, wo_hbm,
    mix_hbm, moe_hbm,
    q_v, k_v, v_v, g_v, wg_v, wu_v, wd_v, wo_v,
    disp, x_v, hid, ybuf, rbuf, ysend, yrecv, fin, ret, omoe,
    lg, cum, bef, local, state, states, dm, drecv, smsg, srecv, pout, inc, heads_v, obuf,
    ld, ldw, a_s, a_r, gy_s, gy_r, gc_s, gc_r, d_s, d_r, s1_s, s1_r, s2_s, s2_r,
    h_s, h_r, c2_s, c2_r, y2_s, y2_r, r_s, r_r, o_s,
):
    E = lax.axis_size("ep")
    L = lax.axis_size("tp")
    chips = L // 2
    e = lax.axis_index("ep")
    t = lax.axis_index("tp")
    y, c = t // 2, t % 2
    partner = 2 * y + 1 - c
    heads, rows, hd = q_v.shape
    half = hd // 2
    blocks = rows // BLOCK
    steps = heads * blocks
    R = rows // L
    width = heads * hd
    capacity = disp.shape[1]
    D = disp.shape[2]
    NT = D // COLS
    group = E * capacity

    def ahead(k):
        return lax.rem(e + k, E)

    def behind(k):
        return lax.rem(e - k + E, E)

    def chip_ahead(v):
        return lax.rem(y + v, chips)

    def chip_behind(v):
        return lax.rem(y - v + chips, chips)

    def remote(src, dst, ss, rs, dev):
        return pltpu.make_async_remote_copy(
            src_ref=src, dst_ref=dst, send_sem=ss, recv_sem=rs,
            device_id=dev, device_id_type=MESH,
        )

    def load_head(i, src, dst, h):
        return pltpu.make_async_copy(src.at[:, h * hd : (h + 1) * hd], dst.at[h], ld.at[i, h])

    def load_weight(i):
        pairs = ((wg_hbm.at[0], wg_v), (wu_hbm.at[0], wu_v), (wd_hbm.at[0], wd_v), (wo_hbm, wo_v))
        return pltpu.make_async_copy(pairs[i][0], pairs[i][1], ldw.at[i])

    def token(k):
        return remote(disp.at[ahead(k)], x_v.at[t, e], a_s.at[k], a_r.at[k], {"ep": ahead(k)})

    def across(v, k):
        p = behind(k)
        dev = {"tp": 2 * chip_ahead(v) + c}
        return remote(x_v.at[t, p], x_v.at[t, p], gy_s.at[v, k], gy_r.at[v, k], dev)

    def beside(v, k):
        p = behind(k)
        g = 2 * chip_behind(v) + c
        return remote(x_v.at[g, p], x_v.at[g, p], gc_s.at[v, k], gc_r.at[v, k], {"tp": partner})

    def decay(k):
        return remote(dm, drecv.at[e], d_s.at[k], d_r.at[k], {"ep": ahead(k)})

    def scatter(h, k):
        return remote(
            smsg.at[h, ahead(k)], srecv.at[h, e], s1_s.at[h, k], s1_r.at[h, k], {"ep": ahead(k)}
        )

    def spread(h, k):
        return remote(
            pout.at[h, ahead(k)], inc.at[h, e], s2_s.at[h, k], s2_r.at[h, k], {"ep": ahead(k)}
        )

    def lane_ahead(i):
        v, flip = i // 2, i % 2
        return 2 * chip_ahead(v) + c + flip * (1 - 2 * c)

    def head_copy(h, i):
        d = lane_ahead(i)
        return remote(
            g_v.at[h, pl.ds(pl.multiple_of(d * R, R), R)],
            heads_v.at[:, pl.ds(pl.multiple_of(t * width + h * hd, hd), hd)],
            h_s.at[h, i], h_r.at[h, i], {"tp": d},
        )

    def core_sum(n, yy):
        return remote(
            ybuf.at[n, 2 * yy + 1 - c], rbuf.at[n, yy], c2_s.at[n, yy], c2_r.at[n, yy],
            {"tp": partner},
        )

    def chip_sum(n, v):
        return remote(
            ysend.at[n, v - 1], yrecv.at[n, v - 1], y2_s.at[n, v], y2_r.at[n, v],
            {"tp": 2 * chip_ahead(v) + c},
        )

    def back(n, k):
        return remote(
            fin.at[n, ahead(k)], ret.at[n, e], r_s.at[n, k], r_r.at[n, k], {"ep": ahead(k)}
        )

    for h in range(heads):
        for i, (src, dst) in enumerate(((q_hbm, q_v), (k_hbm, k_v), (v_hbm, v_v))):
            load_head(i, src, dst, h).start()
    barrier = pltpu.get_barrier_semaphore()
    for k in range(1, E):
        pl.semaphore_signal(barrier, inc=1, device_id={"ep": ahead(k)}, device_id_type=MESH)
    for i in range(1, L):
        pl.semaphore_signal(barrier, inc=1, device_id={"tp": lane_ahead(i)}, device_id_type=MESH)

    floats = x_ref[...].astype(F32)
    scale = lax.rsqrt(jnp.mean(floats * floats, axis=-1, keepdims=True) + norm_eps)
    normed = (floats * scale * mgain_ref[...]).astype(BF16)
    chosen, first = slots_of(ids_ref[...], capacity, group)
    disp[...] = dot(chosen.astype(BF16), normed).astype(BF16).reshape(disp.shape)

    lg[...] = jnp.zeros_like(lg)
    for h in range(heads):
        for b in range(blocks):
            i = h * blocks + b
            lg[i : i + 1, :] = logs_ref[h : h + 1, b * BLOCK : (b + 1) * BLOCK]
    upper = jnp.where(
        lax.broadcasted_iota(jnp.int32, (BLOCK, BLOCK), 0)
        <= lax.broadcasted_iota(jnp.int32, (BLOCK, BLOCK), 1),
        1.0,
        0.0,
    ).astype(BF16)
    la, lb, lc = split3(lg[...])
    sums = dot(la, upper) + dot(lb, upper) + dot(lc, upper)
    cum[...] = sums
    lasts = sums[:, BLOCK - 1 : BLOCK]
    bef[...] = jnp.zeros_like(bef)
    dm[...] = jnp.zeros_like(dm)
    for h in range(heads):
        total = jnp.zeros((1, 1), F32)
        for b in range(blocks):
            i = h * blocks + b
            bef[i : i + 1, :] = jnp.exp(jnp.broadcast_to(total, (1, hd)))
            total = total + lasts[i : i + 1]
        dm[h : h + 1, :] = jnp.exp(jnp.broadcast_to(total, (1, hd)))

    pl.semaphore_wait(barrier, E - 1 + L - 1)
    for k in range(1, E):
        token(k).start()
    x_v[t, e] = disp[e]
    for v in range(1, chips):
        across(v, 0).start()
    beside(0, 0).start()
    for k in range(1, E):
        decay(k).start()
    drecv[e] = dm[...]
    load_weight(0).start()
    load_weight(1).start()
    for h in range(heads):
        load_head(3, g_hbm, g_v, h).start()
    load_weight(2).start()
    load_weight(3).start()

    per_step = -(-(E - 1) // max(steps - 1, 1))

    def pass_on(k):
        token(k).wait_recv()
        for v in range(1, chips):
            across(v, k).start()
        beside(0, k).start()

    def hand_over(k):
        for v in range(1, chips):
            across(v, k).wait_recv()
            beside(v, k).start()

    def prefix(h):
        if h == 0:
            for k in range(1, E):
                decay(k).wait_recv()
        for k in range(1, E):
            scatter(h, k).wait_recv()
        carry = jnp.zeros(srecv.shape[2:], F32)
        for p in range(E):
            pout[h, p] = carry.astype(BF16)
            carry = drecv[p, h : h + 1, :] * carry + srecv[h, p].astype(F32)
        for k in range(1, E):
            spread(h, k).start()
        inc[h, e] = pout[h, e]

    def retention(j):
        h, b = j // blocks, j % blocks

        @pl.when(b == 0)
        def _():
            state[...] = jnp.zeros_like(state)
            for hh in range(heads):

                @pl.when(h == hh)
                def _():
                    for i, (src, dst) in enumerate(((q_hbm, q_v), (k_hbm, k_v), (v_hbm, v_v))):
                        load_head(i, src, dst, hh).wait()

        at = pl.ds(pl.multiple_of(b * BLOCK, BLOCK), BLOCK)
        cum_row = cum[pl.ds(j, 1), :]
        cum_col = jnp.transpose(jnp.broadcast_to(cum_row, (8, BLOCK)))[:, 0:1]
        last = cum_row[:, BLOCK - 1 : BLOCK]
        cb, sb = cos_b[e * blocks + b], sin_b[e * blocks + b]
        cosine = cos_r[...] * cb - sin_r[...] * sb
        sine = sin_r[...] * cb + cos_r[...] * sb

        def rotate(x):
            front = x[:, :half].astype(F32)
            back_half = x[:, half:].astype(F32)
            return jnp.concatenate(
                [front * cosine - back_half * sine, back_half * cosine + front * sine], axis=1
            )

        q_rot = rotate(q_v[h, at, :]).astype(BF16)
        k_rot = (rotate(k_v[h, at, :]) * hd ** (-0.5)).astype(BF16)
        value = v_v[h, at, :]
        q_v[h, at, :] = (q_rot.astype(F32) * jnp.exp(cum_col)).astype(BF16)
        old = state[...]
        states[j] = old
        step = BLOCK // 2
        for i in range(2):
            r0, reach = i * step, (i + 1) * step
            scores = dot(q_rot[r0 : r0 + step], k_rot[:reach], 1, 1)
            causal = (
                lax.broadcasted_iota(jnp.int32, (step, reach), 0) + r0
                >= lax.broadcasted_iota(jnp.int32, (step, reach), 1)
            )
            gap = cum_col[r0 : r0 + step] - cum_row[:, :reach]
            mask = jnp.exp(jnp.where(causal, gap, -1e30))
            weights = (scores * mask).astype(BF16)
            local[j, r0 : r0 + step, :] = dot(weights, value[:reach])
        k_decayed = (k_rot.astype(F32) * jnp.exp(last - cum_col)).astype(BF16)
        fresh = jnp.exp(last) * old + dot(k_decayed, value, 0, 0)
        state[...] = fresh

        for hh in range(heads):

            @pl.when(j == (hh + 1) * blocks - 1)
            def _():
                smsg[hh] = fresh.astype(BF16).reshape(smsg.shape[1:])
                for k in range(1, E):
                    scatter(hh, k).start()
                srecv[hh, e] = smsg[hh, e]

        for i in range(per_step):
            k = 1 + j * per_step + i

            @pl.when(k < E)
            def _():
                pass_on(k)

        for i in range(per_step):
            k = 1 + (j - 1) * per_step + i

            @pl.when((j > 0) & (k < E))
            def _():
                hand_over(k)

        @pl.when(j == 0)
        def _():
            hand_over(0)

        for hh in range(heads - 1):

            @pl.when(j == (hh + 1) * blocks + 2)
            def _():
                prefix(hh)

    loop(steps, retention)
    for i in range(per_step):
        k = 1 + (steps - 1) * per_step + i
        if k < E:
            hand_over(k)

    def finish(h):
        for k in range(1, E):
            spread(h, k).wait_recv()
        load_head(3, g_hbm, g_v, h).wait()
        incoming = inc[h].astype(F32).reshape(hd, hd)
        gain = rgain_ref[:, h * hd : (h + 1) * hd]

        def piece(n):
            i = lax.rem(n + 2, L)
            d = lane_ahead(i)
            j = h * blocks + d * R // BLOCK
            at = pl.ds(pl.multiple_of(d * R, R), R)
            inner = pl.ds(pl.multiple_of(lax.rem(d * R, BLOCK), R), R)
            start = bef[pl.ds(j, 1), :] * incoming + states[j]
            retained = local[j, inner, :] + dot(q_v[h, at, :], start.astype(BF16))
            scale = lax.rsqrt(jnp.mean(retained * retained, axis=-1, keepdims=True) + norm_eps)
            gate = g_v[h, at, :].astype(F32)
            gate = gate / (1.0 + jnp.exp(-gate))
            out = (gate * retained * scale * gain).astype(BF16)
            g_v[h, at, :] = out

            @pl.when(i != 0)
            def _():
                head_copy(h, i).start()

            @pl.when(i == 0)
            def _():
                heads_v[:, pl.ds(pl.multiple_of(t * width + h * hd, hd), hd)] = out

        loop(L, piece)

    for v in range(chips):
        for k in range(E):
            beside(v, k).wait_recv()
    load_weight(0).wait()
    load_weight(1).wait()
    hidden_width = hid.shape[1]
    tile = 256 if hidden_width % 256 == 0 else 128

    def up(n):
        for h in range(heads):

            @pl.when(n == 5 - 4 * (heads - 1 - h))
            def _():
                finish(h)

        @pl.when(n == 2)
        def _():
            prefix(heads - 1)

        at = pl.ds(pl.multiple_of(n * tile, tile), tile)
        x = x_v[...].reshape(L * group, D)
        gate = dot(x, wg_v[:, at])
        rise = dot(x, wu_v[:, at])
        hid[:, at] = (gate / (1.0 + jnp.exp(-gate)) * rise).astype(BF16)

    loop(hidden_width // tile, up)

    load_weight(2).wait()

    def share(n):
        for yy in range(chips):
            core_sum(n, yy).wait_recv()
        for v in range(1, chips):
            yy = chip_ahead(v)
            total = ybuf[n, 2 * yy + c].astype(F32) + rbuf[n, yy].astype(F32)
            ysend[n, v - 1] = total.astype(BF16)
            chip_sum(n, v).start()

    def down(n):
        at = pl.ds(pl.multiple_of(n * COLS, COLS), COLS)
        ybuf[n] = dot(hid[...], wd_v[:, at]).astype(BF16).reshape(ybuf.shape[1:])
        for yy in range(chips):
            core_sum(n, yy).start()

        @pl.when(n > 0)
        def _():
            share(n - 1)

    loop(NT, down)
    share(NT - 1)

    load_weight(3).wait()
    for h in range(heads):
        for i in range(1, L):
            head_copy(h, i).wait_recv()

    def out_copy(n):
        at = pl.ds(pl.multiple_of(n * COLS, COLS), COLS)
        return pltpu.make_async_copy(obuf.at[n], mix_hbm.at[:, at], o_s.at[n])

    def project(n):
        at = pl.ds(pl.multiple_of(n * COLS, COLS), COLS)
        obuf[n] = dot(heads_v[...], wo_v[:, at]).astype(BF16)
        out_copy(n).start()
        total = ybuf[n, t].astype(F32) + rbuf[n, y].astype(F32)
        for v in range(1, chips):
            chip_sum(n, v).wait_recv()
            total = total + yrecv[n, v - 1].astype(F32)
        fin[n] = total.astype(BF16).reshape(fin.shape[1:])
        for k in range(1, E):
            back(n, k).start()
        ret[n, e] = fin[n, e]

    loop(NT, project)

    weight = chosen * jnp.where(first, rw_ref[0:1, :], rw_ref[1:2, :])
    terms = split3(weight)
    for n in range(NT):
        for k in range(1, E):
            back(n, k).wait_recv()
        got = ret[n].reshape(group, COLS)
        total = dot(terms[0], got, 0, 0) + dot(terms[1], got, 0, 0) + dot(terms[2], got, 0, 0)
        omoe[:, n * COLS : (n + 1) * COLS] = total.astype(BF16)
    moe_copy = pltpu.make_async_copy(omoe, moe_hbm, o_s.at[NT])
    moe_copy.start()

    for k in range(1, E):
        token(k).wait_send()
        decay(k).wait_send()
        for h in range(heads):
            scatter(h, k).wait_send()
            spread(h, k).wait_send()
        for n in range(NT):
            back(n, k).wait_send()
    for k in range(E):
        for v in range(1, chips):
            across(v, k).wait_send()
        for v in range(chips):
            beside(v, k).wait_send()
    for h in range(heads):
        for i in range(1, L):
            head_copy(h, i).wait_send()
    for n in range(NT):
        for yy in range(chips):
            core_sum(n, yy).wait_send()
        for v in range(1, chips):
            chip_sum(n, v).wait_send()
        out_copy(n).wait()
    moe_copy.wait()


def on_device(
    mix_query, mix_key, mix_value, mix_gate, log_decay, ret_gain, w_out,
    moe_in, route_ids, route_weights, moe_gain, w_gate, w_up, w_down,
):
    E = lax.axis_size("ep")
    L = lax.axis_size("tp")
    chips = L // 2
    rows, width = mix_query.shape
    heads = width // HEAD_DIM
    blocks = rows // BLOCK
    steps = heads * blocks
    half = HEAD_DIM // 2
    tokens, D = moe_in.shape
    capacity = 4 * tokens // E
    group = E * capacity
    hidden = w_gate.shape[2]
    NT = D // COLS
    R = rows // L
    part = HEAD_DIM // E
    inverse = 10000.0 ** (-(np.arange(half) * 2.0) / HEAD_DIM)
    fine = np.arange(BLOCK)[:, None] * inverse[None, :]
    coarse = (np.arange(E * blocks) * BLOCK)[:, None, None] * inverse[None, None, :]
    tables = [np.asarray(f(x), np.float32) for x in (fine, coarse) for f in (np.cos, np.sin)]
    vm = pl.BlockSpec(memory_space=pltpu.VMEM)
    hbm = pl.BlockSpec(memory_space=pl.ANY)
    pad = -(-steps // 8) * 8
    V = pltpu.VMEM
    S = pltpu.SemaphoreType.DMA
    return pl.pallas_call(
        layer_kernel,
        in_specs=[vm] * 10 + [hbm] * 8,
        out_specs=[hbm, hbm],
        out_shape=[
            jax.ShapeDtypeStruct((R, D), BF16),
            jax.ShapeDtypeStruct((tokens, D), BF16),
        ],
        scratch_shapes=[
            V((heads, rows, HEAD_DIM), BF16), V((heads, rows, HEAD_DIM), BF16),
            V((heads, rows, HEAD_DIM), BF16), V((heads, rows, HEAD_DIM), BF16),
            V((D, hidden), BF16), V((D, hidden), BF16), V((hidden, D), BF16), V(w_out.shape, BF16),
            V((E, capacity, D), BF16), V((L, E, capacity, D), BF16), V((L * group, hidden), BF16),
            V((NT, L, group, COLS), BF16), V((NT, chips, group, COLS), BF16),
            V((NT, chips - 1, group, COLS), BF16), V((NT, chips - 1, group, COLS), BF16),
            V((NT, E, capacity, COLS), BF16), V((NT, E, capacity, COLS), BF16),
            V((tokens, D), BF16),
            V((pad, BLOCK), F32), V((pad, BLOCK), F32), V((pad, HEAD_DIM), F32),
            V((steps, BLOCK, HEAD_DIM), F32), V((HEAD_DIM, HEAD_DIM), F32),
            V((steps, HEAD_DIM, HEAD_DIM), F32),
            V((8, HEAD_DIM), F32), V((E, 8, HEAD_DIM), F32),
            V((heads, E, part, HEAD_DIM), BF16), V((heads, E, part, HEAD_DIM), BF16),
            V((heads, E, part, HEAD_DIM), BF16), V((heads, E, part, HEAD_DIM), BF16),
            V((R, D), BF16), V((NT, R, COLS), BF16),
            S((4, heads)), S((4,)), S((E,)), S((E,)),
            S((chips, E)), S((chips, E)), S((chips, E)), S((chips, E)),
            S((E,)), S((E,)), S((heads, E)), S((heads, E)), S((heads, E)), S((heads, E)),
            S((heads, L)), S((heads, L)), S((NT, chips)), S((NT, chips)),
            S((NT, chips)), S((NT, chips)), S((NT, E)), S((NT, E)), S((NT + 1,)),
        ],
        compiler_params=pltpu.CompilerParams(
            collective_id=0, has_side_effects=True, vmem_limit_bytes=VMEM_LIMIT
        ),
        name="layer",
    )(
        moe_in, route_ids.T, route_weights.T, moe_gain.reshape(1, -1), ret_gain.reshape(1, -1),
        log_decay.T, *tables,
        mix_query, mix_key, mix_value, mix_gate, w_gate, w_up, w_down, w_out,
    )


def solution(mesh):
    in_specs = (
        P("ep", "tp"),
        P("ep", "tp"),
        P("ep", "tp"),
        P("ep", "tp"),
        P("ep", "tp"),
        P("tp"),
        P(),
        P(("ep", "tp"), None),
        P(("ep", "tp"), None),
        P(("ep", "tp"), None),
        P(),
        P("ep", None, "tp"),
        P("ep", None, "tp"),
        P("ep", "tp", None),
    )
    out_specs = (P(("ep", "tp"), None), P(("ep", "tp"), None))
    return jax.shard_map(
        lambda *args: tuple(on_device(*args)), mesh=mesh, in_specs=in_specs, out_specs=out_specs,
        check_vma=False,
    )
```

```python
import functools

import jax
import jax.numpy as jnp
import numpy as np
from jax import lax
from jax.experimental import pallas as pl
from jax.experimental.pallas import tpu as pltpu
from jax.sharding import PartitionSpec as P

HEAD_DIM = 256
BLOCK = 512
norm_eps = 1e-06
F32 = jnp.float32
BF16 = jnp.bfloat16
MESH = pl.DeviceIdType.MESH
VMEM_LIMIT = 63000000
COLS = 512


def dot(a, b, ca=1, cb=0):
    return lax.dot_general(a, b, (((ca,), (cb,)), ((), ())), preferred_element_type=F32)


def split3(x):
    a = x.astype(BF16)
    rest = x - a.astype(F32)
    b = rest.astype(BF16)
    c = (rest - b.astype(F32)).astype(BF16)
    return a, b, c


def loop(count, body):
    def step(i, carry):
        body(i)
        return carry

    lax.fori_loop(0, count, step, 0)


def slots_of(ids, capacity, count):
    tokens = ids.shape[1]
    row = lax.broadcasted_iota(jnp.int32, (count, tokens), 0)
    expert = row // capacity
    first = ids[0:1, :] == expert
    second = ids[1:2, :] == expert
    member = jnp.where(first | second, 1.0, 0.0)
    earlier = jnp.where(
        lax.broadcasted_iota(jnp.int32, (tokens, tokens), 0)
        < lax.broadcasted_iota(jnp.int32, (tokens, tokens), 1),
        1.0,
        0.0,
    ).astype(BF16)
    taken = dot(member.astype(BF16), earlier)
    slot = (row - expert * capacity).astype(F32)
    return jnp.where(taken == slot, member, 0.0), first


def layer_kernel(
    x_hbm, ids_hbm, rw_hbm, mgain_hbm, rgain_hbm, logs_hbm, cosr_hbm, sinr_hbm, cosb_hbm, sinb_hbm,
    q_hbm, k_hbm, v_hbm, g_hbm, wg_hbm, wu_hbm, wd_hbm, wo_hbm,
    obuf, omoe,
    x_ref, ids_ref, rw_ref, mgain_ref, rgain_ref, logs_ref, cos_r, sin_r, cos_b, sin_b,
    q_v, k_v, v_v, g_v, wg_v, wu_v, wd_v, wo_v,
    disp, x_v, hid, ybuf, rbuf, ysend, yrecv, fin, ret,
    lg, cum, bef, local, state, states, dm, drecv, smsg, srecv, tsend, trecv, pout, inc, heads_v, hlast,
    lds, ld, ldw, a_s, a_r, gy_s, gy_r, gc_s, gc_r, d_s, d_r, s1_s, s1_r, t_s, t_r, s2_s, s2_r,
    h_s, h_r, c2_s, c2_r, y2_s, y2_r, r_s, r_r,
):
    E = lax.axis_size("ep")
    L = lax.axis_size("tp")
    chips = L // 2
    e = lax.axis_index("ep")
    t = lax.axis_index("tp")
    y, c = t // 2, t % 2
    partner = 2 * y + 1 - c
    heads, rows, hd = q_v.shape
    half = hd // 2
    blocks = rows // BLOCK
    steps = heads * blocks
    R = rows // L
    width = heads * hd
    capacity = disp.shape[1]
    D = disp.shape[2]
    NT = D // COLS
    group = E * capacity

    def ahead(k):
        return lax.rem(e + k, E)

    G = E // 2
    upper_half, place = e // G, e % G

    def flip(k):
        out, bit = 0, 1
        while bit < E:
            out = out + bit * ((e // bit + k // bit) % 2)
            bit *= 2
        return out

    def member(k):
        return upper_half * G + lax.rem(place + k, G)

    def chip_ahead(v):
        return lax.rem(y + v, chips)

    def chip_behind(v):
        return lax.rem(y - v + chips, chips)

    def remote(src, dst, ss, rs, dev):
        return pltpu.make_async_remote_copy(
            src_ref=src, dst_ref=dst, send_sem=ss, recv_sem=rs,
            device_id=dev, device_id_type=MESH,
        )

    def load_head(i, src, dst, h):
        return pltpu.make_async_copy(src.at[:, h * hd : (h + 1) * hd], dst.at[h], ld.at[i, h])

    def load_weight(i):
        pairs = ((wg_hbm.at[0], wg_v), (wu_hbm.at[0], wu_v), (wd_hbm.at[0], wd_v), (wo_hbm, wo_v))
        return pltpu.make_async_copy(pairs[i][0], pairs[i][1], ldw.at[i])

    def token(k):
        return remote(disp.at[flip(k)], x_v.at[t, e], a_s, a_r.at[k], {"ep": flip(k)})

    def across(v, k):
        p = flip(k)
        dev = {"tp": 2 * chip_ahead(v) + c}
        return remote(x_v.at[t, p], x_v.at[t, p], gy_s, gy_r.at[v - 1, k], dev)

    def beside(v, k):
        p = flip(k)
        g = 2 * chip_behind(v) + c
        return remote(x_v.at[g, p], x_v.at[g, p], gc_s, gc_r, {"tp": partner})

    def decay(k):
        return remote(dm, drecv.at[place], d_s, d_r, {"ep": member(k)})

    def scatter(h, k):
        return remote(
            smsg.at[h, lax.rem(place + k, G)], srecv.at[h, place], s1_s.at[h], s1_r.at[h],
            {"ep": member(k)},
        )

    def lift(h):
        return remote(tsend.at[h], trecv.at[h], t_s, t_r.at[h], {"ep": lax.rem(e + G, E)})

    def spread(h, k):
        return remote(
            pout.at[h, lax.rem(place + k, G)], inc.at[h, place], s2_s.at[h], s2_r.at[h],
            {"ep": member(k)},
        )

    def lane_ahead(i):
        v, flip = i // 2, i % 2
        return 2 * chip_ahead(v) + c + flip * (1 - 2 * c)

    def last_copy():
        d = lane_ahead(L - 1)
        return remote(
            g_v.at[heads - 1, pl.ds(pl.multiple_of(d * R, R), R)], hlast,
            h_s.at[heads - 1], h_r.at[1], {"tp": d},
        )

    last_source = 2 * chip_behind(chips - 1) + 1 - c
    last_rows = pl.ds(pl.multiple_of(last_source * width + (heads - 1) * hd, hd), hd)

    def head_copy(h, i):
        d = lane_ahead(i)
        return remote(
            g_v.at[h, pl.ds(pl.multiple_of(d * R, R), R)],
            heads_v.at[:, pl.ds(pl.multiple_of(t * width + h * hd, hd), hd)],
            h_s.at[h], h_r.at[0], {"tp": d},
        )

    def core_sum(n, yy):
        return remote(
            ybuf.at[n, 2 * yy + 1 - c], rbuf.at[n, yy], c2_s, c2_r.at[n],
            {"tp": partner},
        )

    def chip_sum(n, v):
        return remote(
            ysend.at[n, v - 1], yrecv.at[n, v - 1], y2_s, y2_r.at[n],
            {"tp": 2 * chip_ahead(v) + c},
        )

    def back(n, k):
        return remote(
            fin.at[n, ahead(k)], ret.at[n, e], r_s.at[n], r_r.at[n], {"ep": ahead(k)}
        )

    barrier = pltpu.get_barrier_semaphore()
    for k in range(1, E):
        pl.semaphore_signal(barrier, inc=1, device_id={"ep": flip(k)}, device_id_type=MESH)
    for i in range(1, L):
        pl.semaphore_signal(barrier, inc=1, device_id={"tp": lane_ahead(i)}, device_id_type=MESH)

    def done(ref, sem):
        pltpu.make_async_copy(ref, ref, sem).wait()

    small = [
        pltpu.make_async_copy(src, dst, lds.at[i])
        for i, (src, dst) in enumerate(
            (
                (x_hbm, x_ref), (mgain_hbm, mgain_ref), (ids_hbm, ids_ref), (logs_hbm, logs_ref),
                (cosr_hbm, cos_r), (sinr_hbm, sin_r), (cosb_hbm, cos_b), (sinb_hbm, sin_b),
                (rgain_hbm, rgain_ref), (rw_hbm, rw_ref),
            )
        )
    ]
    for copy in small:
        copy.start()
    for copy in small[:3]:
        copy.wait()
    for h in range(heads):
        for i, (src, dst) in ((1, (k_hbm, k_v)), (2, (v_hbm, v_v))):
            load_head(i, src, dst, h).start()
    for h in range(heads):
        load_head(0, q_hbm, q_v, h).start()

    floats = x_ref[...].astype(F32)
    scale = lax.rsqrt(jnp.mean(floats * floats, axis=-1, keepdims=True) + norm_eps)
    normed = (floats * scale * mgain_ref[...]).astype(BF16)
    chosen, first = slots_of(ids_ref[...], capacity, group)
    disp[...] = dot(chosen.astype(BF16), normed).astype(BF16).reshape(disp.shape)

    for copy in small[3:]:
        copy.wait()
    lg[...] = jnp.zeros_like(lg)
    for h in range(heads):
        for b in range(blocks):
            i = h * blocks + b
            lg[i : i + 1, :] = logs_ref[h : h + 1, b * BLOCK : (b + 1) * BLOCK]
    upper = jnp.where(
        lax.broadcasted_iota(jnp.int32, (BLOCK, BLOCK), 0)
        <= lax.broadcasted_iota(jnp.int32, (BLOCK, BLOCK), 1),
        1.0,
        0.0,
    ).astype(BF16)
    la, lb, lc = split3(lg[...])
    sums = dot(la, upper) + dot(lb, upper) + dot(lc, upper)
    cum[...] = sums
    lasts = sums[:, BLOCK - 1 : BLOCK]
    bef[...] = jnp.zeros_like(bef)
    dm[...] = jnp.zeros_like(dm)
    for h in range(heads):
        total = jnp.zeros((1, 1), F32)
        for b in range(blocks):
            i = h * blocks + b
            bef[i : i + 1, :] = jnp.exp(jnp.broadcast_to(total, (1, hd)))
            total = total + lasts[i : i + 1]
        dm[h : h + 1, :] = jnp.exp(jnp.broadcast_to(total, (1, hd)))

    pl.semaphore_wait(barrier, E - 1 + L - 1)
    mids = list(range(E - E // 4, E)) + list(range(E // 2, E - E // 4))
    near = list(range(2, E // 2))
    n4 = len(mids) // 4
    waves = [
        [1] + near[:1] + mids[:n4],
        mids[n4 : 2 * n4],
        near[1:],
        mids[2 * n4 :],
    ]
    order = [0] + waves[0] + waves[1] + waves[2] + waves[3]

    held = len(waves[3])

    def send_wave(i):
        for k in waves[i]:
            token(k).start()

    def pass_on(k):
        token(k).wait_recv()
        for v in range(1, chips):
            across(v, k).start()
        beside(0, k).start()

    def hand_over(k):
        for v in range(1, chips):
            across(v, k).wait_recv()
            beside(v, k).start()

    send_wave(0)
    x_v[t, e] = disp[e]
    for v in range(1, chips):
        across(v, 0).start()
    beside(0, 0).start()
    for k in range(1, G):
        decay(k).start()
    drecv[place] = dm[...]

    def tables_of(b):
        cb, sb = cos_b[e * blocks + b], sin_b[e * blocks + b]
        return cos_r[...] * cb - sin_r[...] * sb, sin_r[...] * cb + cos_r[...] * sb

    def rotate(x, cosine, sine):
        front = x[:, :half].astype(F32)
        rest = x[:, half:].astype(F32)
        return jnp.concatenate([front * cosine - rest * sine, rest * cosine + front * sine], axis=1)

    def column(row):
        return jnp.transpose(jnp.broadcast_to(row, (8, BLOCK)))[:, 0:1]

    def rows_of(b):
        return pl.ds(pl.multiple_of(b * BLOCK, BLOCK), BLOCK)

    for h in range(heads):
        load_head(1, k_hbm, k_v, h).wait()
        load_head(2, v_hbm, v_v, h).wait()
        state[...] = jnp.zeros_like(state)

        def update(b):
            j = h * blocks + b
            at = rows_of(b)
            cum_row = cum[pl.ds(j, 1), :]
            last = cum_row[:, BLOCK - 1 : BLOCK]
            k_rot = (rotate(k_v[h, at, :], *tables_of(b)) * hd ** (-0.5)).astype(BF16)
            k_v[h, at, :] = k_rot
            k_decayed = (k_rot.astype(F32) * jnp.exp(last - column(cum_row))).astype(BF16)
            old = state[...]
            states[j] = old
            state[...] = jnp.exp(last) * old + dot(k_decayed, v_v[h, at, :], 0, 0)
            if h == heads - 1:
                for k, step in ((order[1], 1), (order[2], blocks - 1)):

                    @pl.when(b == step)
                    def _():
                        pass_on(k)

        loop(blocks, update)
        smsg[h] = state[...].astype(BF16).reshape(smsg.shape[1:])
        for k in range(1, G):
            scatter(h, k).start()
        srecv[h, place] = smsg[h, place]
        if h == 0:
            send_wave(1)
    load_weight(0).start()
    load_weight(1).start()
    for h in range(heads):
        load_head(3, g_hbm, g_v, h).start()
    load_weight(2).start()
    load_weight(3).start()

    def scan(h, carry):
        for p in range(G):
            pout[h, p] = carry.astype(BF16)
            carry = drecv[p, h : h + 1, :] * carry + srecv[h, p].astype(F32)
        for k in range(1, G):
            spread(h, k).start()
        inc[h, place] = pout[h, place]
        return carry

    def arrivals(h):
        if h == 0:
            done(drecv.at[0 : G - 1], d_r)
        done(srecv.at[h, 0 : G - 1], s1_r.at[h])

    def prefix_low(h):
        @pl.when(upper_half == 0)
        def _():
            arrivals(h)
            carry = scan(h, jnp.zeros(srecv.shape[2:], F32))
            tsend[h] = carry.astype(BF16)
            lift(h).start()

    def prefix_high(h):
        @pl.when(upper_half == 1)
        def _():
            arrivals(h)
            lift(h).wait_recv()
            scan(h, trecv[h].astype(F32))

    def within(j):
        h, b = j // blocks, j % blocks
        for hh in range(heads):

            @pl.when(j == hh * blocks)
            def _():
                load_head(0, q_hbm, q_v, hh).wait()

        at = rows_of(b)
        cum_row = cum[pl.ds(j, 1), :]
        cum_col = column(cum_row)
        q_rot = rotate(q_v[h, at, :], *tables_of(b)).astype(BF16)
        k_rot = k_v[h, at, :]
        value = v_v[h, at, :]
        q_v[h, at, :] = (q_rot.astype(F32) * jnp.exp(cum_col)).astype(BF16)
        step = BLOCK // 2
        for i in range(2):
            r0, reach = i * step, (i + 1) * step
            scores = dot(q_rot[r0 : r0 + step], k_rot[:reach], 1, 1)
            causal = (
                lax.broadcasted_iota(jnp.int32, (step, reach), 0) + r0
                >= lax.broadcasted_iota(jnp.int32, (step, reach), 1)
            )
            gap = cum_col[r0 : r0 + step] - cum_row[:, :reach]
            mask = jnp.exp(jnp.where(causal, gap, -1e30))
            weights = (scores * mask).astype(BF16)
            local[j, r0 : r0 + step, :] = dot(weights, value[:reach])

        for i, k in enumerate(order[3:-held]):

            @pl.when(j == min(1 + 2 * i + i // 2, steps - 1))
            def _():
                pass_on(k)

        for i, k in enumerate(order[:2]):

            @pl.when(j == steps // 2 + min(2 * i, steps // 2 - 1))
            def _():
                hand_over(k)

        for hh in range(heads):
            if high_step(hh) < steps:

                @pl.when(j == high_step(hh))
                def _():
                    prefix_high(hh)

            @pl.when(j == low_step(hh))
            def _():
                prefix_low(hh)
                if hh == 0:
                    send_wave(2)
                if hh == heads - 1:
                    send_wave(3)

    def low_step(h):
        return min(max(0, 3 - 3 * (heads - 1 - h)), steps - 1)

    def high_step(h):
        return low_step(h) + 4

    loop(steps, within)
    for h in range(heads):
        if high_step(h) >= steps:
            prefix_high(h)

    def finish(h):
        done(inc.at[h, 0 : G - 1], s2_r.at[h])
        load_head(3, g_hbm, g_v, h).wait()
        incoming = inc[h].astype(F32).reshape(hd, hd)
        gain = rgain_ref[:, h * hd : (h + 1) * hd]

        def piece(n):
            i = lax.rem(n + 2, L)
            d = lane_ahead(i)
            j = h * blocks + d * R // BLOCK
            at = pl.ds(pl.multiple_of(d * R, R), R)
            inner = pl.ds(pl.multiple_of(lax.rem(d * R, BLOCK), R), R)
            start = bef[pl.ds(j, 1), :] * incoming + states[j]
            retained = local[j, inner, :] + dot(q_v[h, at, :], start.astype(BF16))
            scale = lax.rsqrt(jnp.mean(retained * retained, axis=-1, keepdims=True) + norm_eps)
            gate = g_v[h, at, :].astype(F32)
            gate = gate / (1.0 + jnp.exp(-gate))
            out = (gate * retained * scale * gain).astype(BF16)
            g_v[h, at, :] = out

            @pl.when((i != 0) if h < heads - 1 else ((i != 0) & (i != L - 1)))
            def _():
                head_copy(h, i).start()

            @pl.when(i == 0)
            def _():
                heads_v[:, pl.ds(pl.multiple_of(t * width + h * hd, hd), hd)] = out

        loop(L, piece)

    for k in order[-held:]:
        pass_on(k)
    for h in range(heads):
        finish(h)
        if h == 0:
            for k in order[2:5]:
                hand_over(k)
    for k in order[5:]:
        hand_over(k)

    done(x_v.at[0:chips], gc_r)
    load_weight(0).wait()
    load_weight(1).wait()
    hidden_width = hid.shape[1]
    tile = 256 if hidden_width % 256 == 0 else 128

    def up(n):
        at = pl.ds(pl.multiple_of(n * tile, tile), tile)
        x = x_v[...].reshape(L * group, D)
        both = dot(x, jnp.concatenate([wg_v[:, at], wu_v[:, at]], axis=1))
        gate, rise = both[:, :tile], both[:, tile:]
        hid[:, at] = (gate / (1.0 + jnp.exp(-gate)) * rise).astype(BF16)

    loop(hidden_width // tile, up)

    load_weight(2).wait()

    def share(n):
        done(rbuf.at[n], c2_r.at[n])
        for v in range(1, chips):
            yy = chip_ahead(v)
            total = ybuf[n, 2 * yy + c].astype(F32) + rbuf[n, yy].astype(F32)
            ysend[n, v - 1] = total.astype(BF16)
            chip_sum(n, v).start()

    def down(n):
        at = pl.ds(pl.multiple_of(n * COLS, COLS), COLS)
        ybuf[n] = dot(hid[...], wd_v[:, at]).astype(BF16).reshape(ybuf.shape[1:])
        for yy in range(chips):
            core_sum(n, yy).start()

        @pl.when(n > 0)
        def _():
            share(n - 1)

    loop(NT, down)
    share(NT - 1)
    last_copy().start()

    load_weight(3).wait()
    done(heads_v.at[:, 0 : (heads * (L - 1) - 1) * hd], h_r.at[0])
    heads_v[:, last_rows] = jnp.zeros_like(hlast)

    def parts(n):
        for i in range(2):
            at = (2 * n + i) * R
            rows_at = pl.ds(pl.multiple_of(lax.rem(at, BLOCK), R), R)
            yield at // BLOCK, rows_at, slice(i * hd, (i + 1) * hd)

    def project(n):
        at = pl.ds(pl.multiple_of(n * COLS, COLS), COLS)
        sums = dot(heads_v[...], wo_v[:, at])
        for plane, rows_at, cols in parts(n):
            local[plane, rows_at, :] = sums[:, cols]
        total = ybuf[n, t].astype(F32) + rbuf[n, y].astype(F32)
        done(yrecv.at[n], y2_r.at[n])
        for v in range(1, chips):
            total = total + yrecv[n, v - 1].astype(F32)
        fin[n] = total.astype(BF16).reshape(fin.shape[1:])
        for k in range(1, E):
            back(n, k).start()
        ret[n, e] = fin[n, e]

    loop(NT, project)

    weight = chosen * jnp.where(first, rw_ref[0:1, :], rw_ref[1:2, :])
    terms = split3(weight)
    for n in range(NT):
        done(ret.at[n, 0 : E - 1], r_r.at[n])
        got = ret[n].reshape(group, COLS)
        total = dot(terms[0], got, 0, 0) + dot(terms[1], got, 0, 0) + dot(terms[2], got, 0, 0)
        omoe[:, n * COLS : (n + 1) * COLS] = total.astype(BF16)

    last_copy().wait_recv()

    def project_last(n):
        at = pl.ds(pl.multiple_of(n * COLS, COLS), COLS)
        sums = dot(hlast[...], wo_v[last_rows, at])
        for plane, rows_at, cols in parts(n):
            to = pl.ds(pl.multiple_of(n * COLS + cols.start, hd), hd)
            obuf[:, to] = (local[plane, rows_at, :] + sums[:, cols]).astype(BF16)

    loop(NT, project_last)

    done(x_v.at[0, 0 : E - 1], a_s)
    done(x_v.at[0 : chips - 1], gy_s)
    done(x_v.at[0:chips], gc_s)
    done(drecv.at[0 : G - 1], d_s)

    @pl.when(upper_half == 0)
    def _():
        done(tsend, t_s)

    for h in range(heads):
        done(smsg.at[h, 0 : G - 1], s1_s.at[h])
        done(pout.at[h, 0 : G - 1], s2_s.at[h])
        done(heads_v.at[:, 0 : (L - 1) * hd], h_s.at[h])
    done(rbuf, c2_s)
    done(ysend, y2_s)
    for n in range(NT):
        done(fin.at[n, 0 : E - 1], r_s.at[n])


def on_device(
    mix_query, mix_key, mix_value, mix_gate, log_decay, ret_gain, w_out,
    moe_in, route_ids, route_weights, moe_gain, w_gate, w_up, w_down,
):
    E = lax.axis_size("ep")
    L = lax.axis_size("tp")
    chips = L // 2
    rows, width = mix_query.shape
    heads = width // HEAD_DIM
    blocks = rows // BLOCK
    steps = heads * blocks
    half = HEAD_DIM // 2
    tokens, D = moe_in.shape
    capacity = 4 * tokens // E
    group = E * capacity
    hidden = w_gate.shape[2]
    NT = D // COLS
    R = rows // L
    G = E // 2
    part = HEAD_DIM // G
    inverse = 10000.0 ** (-(np.arange(half) * 2.0) / HEAD_DIM)
    fine = np.arange(BLOCK)[:, None] * inverse[None, :]
    coarse = (np.arange(E * blocks) * BLOCK)[:, None, None] * inverse[None, None, :]
    tables = [np.asarray(f(x), np.float32) for x in (fine, coarse) for f in (np.cos, np.sin)]
    hbm = pl.BlockSpec(memory_space=pl.ANY)
    pad = -(-steps // 8) * 8
    V = pltpu.VMEM
    S = pltpu.SemaphoreType.DMA
    return pl.pallas_call(
        layer_kernel,
        in_specs=[hbm] * 18,
        out_specs=[pl.BlockSpec(memory_space=pltpu.VMEM)] * 2,
        out_shape=[
            pltpu.VMEM((R, D), BF16),
            pltpu.VMEM((tokens, D), BF16),
        ],
        scratch_shapes=[
            V((tokens, D), BF16), V((2, tokens), jnp.int32), V((2, tokens), F32),
            V((1, D), F32), V((1, width), F32), V((heads, rows), F32),
            V((BLOCK, half), F32), V((BLOCK, half), F32),
            V((E * blocks, 1, half), F32), V((E * blocks, 1, half), F32),
            V((heads, rows, HEAD_DIM), BF16), V((heads, rows, HEAD_DIM), BF16),
            V((heads, rows, HEAD_DIM), BF16), V((heads, rows, HEAD_DIM), BF16),
            V((D, hidden), BF16), V((D, hidden), BF16), V((hidden, D), BF16), V(w_out.shape, BF16),
            V((E, capacity, D), BF16), V((L, E, capacity, D), BF16), V((L * group, hidden), BF16),
            V((NT, L, group, COLS), BF16), V((NT, chips, group, COLS), BF16),
            V((NT, chips - 1, group, COLS), BF16), V((NT, chips - 1, group, COLS), BF16),
            V((NT, E, capacity, COLS), BF16), V((NT, E, capacity, COLS), BF16),
            V((pad, BLOCK), F32), V((pad, BLOCK), F32), V((pad, HEAD_DIM), F32),
            V((steps, BLOCK, HEAD_DIM), F32), V((HEAD_DIM, HEAD_DIM), F32),
            V((steps, HEAD_DIM, HEAD_DIM), F32),
            V((8, HEAD_DIM), F32), V((G, 8, HEAD_DIM), F32),
            V((heads, G, part, HEAD_DIM), BF16), V((heads, G, part, HEAD_DIM), BF16),
            V((heads, part, HEAD_DIM), BF16), V((heads, part, HEAD_DIM), BF16),
            V((heads, G, part, HEAD_DIM), BF16), V((heads, G, part, HEAD_DIM), BF16),
            V((R, D), BF16), V((R, HEAD_DIM), BF16),
            S((10,)), S((4, heads)), S((4,)), S(()), S((E,)),
            S(()), S((chips - 1, E)), S(()), S(()),
            S(()), S(()), S((heads,)), S((heads,)), S(()), S((heads,)), S((heads,)), S((heads,)),
            S((heads,)), S((2,)), S(()), S((NT,)), S(()), S((NT,)), S((NT,)), S((NT,)),
        ],
        compiler_params=pltpu.CompilerParams(
            collective_id=0, has_side_effects=True, vmem_limit_bytes=VMEM_LIMIT
        ),
        name="layer",
    )(
        moe_in, route_ids.T, route_weights.T, moe_gain.reshape(1, -1), ret_gain.reshape(1, -1),
        log_decay.T, *tables,
        mix_query, mix_key, mix_value, mix_gate, w_gate, w_up, w_down, w_out,
    )


def solution(mesh):
    in_specs = (
        P("ep", "tp"),
        P("ep", "tp"),
        P("ep", "tp"),
        P("ep", "tp"),
        P("ep", "tp"),
        P("tp"),
        P(),
        P(("ep", "tp"), None),
        P(("ep", "tp"), None),
        P(("ep", "tp"), None),
        P(),
        P("ep", None, "tp"),
        P("ep", None, "tp"),
        P("ep", "tp", None),
    )
    out_specs = (P(("ep", "tp"), None), P(("ep", "tp"), None))
    return jax.shard_map(
        lambda *args: tuple(on_device(*args)), mesh=mesh, in_specs=in_specs, out_specs=out_specs,
        check_vma=False,
    )
```

```python
import functools

import jax
import jax.numpy as jnp
import numpy as np
from jax import lax
from jax.experimental import pallas as pl
from jax.experimental.pallas import tpu as pltpu
from jax.sharding import PartitionSpec as P

HEAD_DIM = 256
BLOCK = 512
norm_eps = 1e-06
F32 = jnp.float32
BF16 = jnp.bfloat16
MESH = pl.DeviceIdType.MESH
VMEM_LIMIT = 63000000
COLS = 512


def dot(a, b, ca=1, cb=0):
    return lax.dot_general(a, b, (((ca,), (cb,)), ((), ())), preferred_element_type=F32)


def split3(x):
    a = x.astype(BF16)
    rest = x - a.astype(F32)
    b = rest.astype(BF16)
    c = (rest - b.astype(F32)).astype(BF16)
    return a, b, c


def loop(count, body, unroll=False):
    def step(i, carry):
        body(i)
        return carry

    lax.fori_loop(0, count, step, 0, unroll=unroll)


def slots_of(ids, capacity, count):
    tokens = ids.shape[1]
    row = lax.broadcasted_iota(jnp.int32, (count, tokens), 0)
    expert = row // capacity
    first = ids[0:1, :] == expert
    second = ids[1:2, :] == expert
    member = jnp.where(first | second, 1.0, 0.0)
    earlier = jnp.where(
        lax.broadcasted_iota(jnp.int32, (tokens, tokens), 0)
        < lax.broadcasted_iota(jnp.int32, (tokens, tokens), 1),
        1.0,
        0.0,
    ).astype(BF16)
    taken = dot(member.astype(BF16), earlier)
    slot = (row - expert * capacity).astype(F32)
    return jnp.where(taken == slot, member, 0.0), first


def layer_kernel(
    x_hbm, ids_hbm, rw_hbm, mgain_hbm, rgain_hbm, logs_hbm, cosr_hbm, sinr_hbm, cosb_hbm, sinb_hbm,
    q_hbm, k_hbm, v_hbm, g_hbm, wg_hbm, wu_hbm, wd_hbm, wo_hbm,
    obuf, omoe,
    x_ref, ids_ref, rw_ref, mgain_ref, rgain_ref, logs_ref, cos_r, sin_r, cos_b, sin_b,
    q_v, k_v, v_v, g_v, wg_v, wu_v, wd_v, wo_v,
    disp, x_v, hid, ybuf, rbuf, ysend, yrecv, fin, ret,
    lg, cum, bef, local, state, states, dm, drecv, smsg, srecv, tsend, trecv, pout, inc, heads_v, hlast,
    lds, ld, ldw, a_s, a_r, gy_s, gy_r, gc_s, gc_r, d_s, d_r, s1_s, s1_r, t_s, t_r, s2_s, s2_r,
    h_s, h_r, c2_s, c2_r, y2_s, y2_r, r_s, r_r,
):
    E = lax.axis_size("ep")
    L = lax.axis_size("tp")
    chips = L // 2
    e = lax.axis_index("ep")
    t = lax.axis_index("tp")
    y, c = t // 2, t % 2
    partner = 2 * y + 1 - c
    heads, rows, hd = q_v.shape
    half = hd // 2
    blocks = rows // BLOCK
    steps = heads * blocks
    R = rows // L
    width = heads * hd
    capacity = disp.shape[1]
    D = disp.shape[2]
    NT = D // COLS
    group = E * capacity

    def ahead(k):
        return lax.rem(e + k, E)

    G = E // 2
    upper_half, place = e // G, e % G

    def flip(k):
        out, bit = 0, 1
        while bit < E:
            out = out + bit * ((e // bit + k // bit) % 2)
            bit *= 2
        return out

    def member(k):
        return upper_half * G + lax.rem(place + k, G)

    def chip_ahead(v):
        return lax.rem(y + v, chips)

    def chip_behind(v):
        return lax.rem(y - v + chips, chips)

    def remote(src, dst, ss, rs, dev):
        return pltpu.make_async_remote_copy(
            src_ref=src, dst_ref=dst, send_sem=ss, recv_sem=rs,
            device_id=dev, device_id_type=MESH,
        )

    def load_head(i, src, dst, h):
        return pltpu.make_async_copy(src.at[:, h * hd : (h + 1) * hd], dst.at[h], ld.at[i, h])

    def load_weight(i):
        pairs = ((wg_hbm.at[0], wg_v), (wu_hbm.at[0], wu_v), (wd_hbm.at[0], wd_v), (wo_hbm, wo_v))
        return pltpu.make_async_copy(pairs[i][0], pairs[i][1], ldw.at[i])

    def token(k):
        return remote(disp.at[flip(k)], x_v.at[t, e], a_s, a_r.at[k], {"ep": flip(k)})

    def across(v, k):
        p = flip(k)
        dev = {"tp": 2 * chip_ahead(v) + c}
        return remote(x_v.at[t, p], x_v.at[t, p], gy_s, gy_r.at[v - 1, k], dev)

    def beside(v, k):
        p = flip(k)
        g = 2 * chip_behind(v) + c
        return remote(x_v.at[g, p], x_v.at[g, p], gc_s, gc_r, {"tp": partner})

    def decay(k):
        return remote(dm, drecv.at[place], d_s, d_r, {"ep": member(k)})

    def scatter(h, k):
        return remote(
            smsg.at[h, lax.rem(place + k, G)], srecv.at[h, place], s1_s.at[h], s1_r.at[h],
            {"ep": member(k)},
        )

    def lift(h):
        return remote(tsend.at[h], trecv.at[h], t_s, t_r.at[h], {"ep": lax.rem(e + G, E)})

    def spread(h, k):
        return remote(
            pout.at[h, lax.rem(place + k, G)], inc.at[h, place], s2_s.at[h], s2_r.at[h],
            {"ep": member(k)},
        )

    def lane_ahead(i):
        v, flip = i // 2, i % 2
        return 2 * chip_ahead(v) + c + flip * (1 - 2 * c)

    def last_copy():
        d = lane_ahead(L - 1)
        return remote(
            g_v.at[heads - 1, pl.ds(pl.multiple_of(d * R, R), R)], hlast,
            h_s.at[heads - 1], h_r.at[1], {"tp": d},
        )

    last_source = 2 * chip_behind(chips - 1) + 1 - c
    last_rows = pl.ds(pl.multiple_of(last_source * width + (heads - 1) * hd, hd), hd)

    def head_copy(h, i):
        d = lane_ahead(i)
        return remote(
            g_v.at[h, pl.ds(pl.multiple_of(d * R, R), R)],
            heads_v.at[:, pl.ds(pl.multiple_of(t * width + h * hd, hd), hd)],
            h_s.at[h], h_r.at[0], {"tp": d},
        )

    def core_sum(n, yy):
        return remote(
            ybuf.at[n, 2 * yy + 1 - c], rbuf.at[n, yy], c2_s, c2_r.at[n],
            {"tp": partner},
        )

    def chip_sum(n, v):
        return remote(
            ysend.at[n, v - 1], yrecv.at[n, v - 1], y2_s, y2_r.at[n],
            {"tp": 2 * chip_ahead(v) + c},
        )

    def back(n, k):
        return remote(
            fin.at[n, ahead(k)], ret.at[n, e], r_s.at[n], r_r.at[n], {"ep": ahead(k)}
        )

    barrier = pltpu.get_barrier_semaphore()
    for k in range(1, E):
        pl.semaphore_signal(barrier, inc=1, device_id={"ep": flip(k)}, device_id_type=MESH)
    for i in range(1, L):
        pl.semaphore_signal(barrier, inc=1, device_id={"tp": lane_ahead(i)}, device_id_type=MESH)

    def done(ref, sem):
        pltpu.make_async_copy(ref, ref, sem).wait()

    small = [
        pltpu.make_async_copy(src, dst, lds.at[i])
        for i, (src, dst) in enumerate(
            (
                (x_hbm, x_ref), (mgain_hbm, mgain_ref), (ids_hbm, ids_ref), (logs_hbm, logs_ref),
                (cosr_hbm, cos_r), (sinr_hbm, sin_r), (cosb_hbm, cos_b), (sinb_hbm, sin_b),
                (rgain_hbm, rgain_ref), (rw_hbm, rw_ref),
            )
        )
    ]
    for copy in small:
        copy.start()
    for copy in small[:3]:
        copy.wait()
    for h in range(heads):
        for i, (src, dst) in ((1, (k_hbm, k_v)), (2, (v_hbm, v_v))):
            load_head(i, src, dst, h).start()
    for h in range(heads):
        load_head(0, q_hbm, q_v, h).start()

    floats = x_ref[...].astype(F32)
    scale = lax.rsqrt(jnp.mean(floats * floats, axis=-1, keepdims=True) + norm_eps)
    normed = (floats * scale * mgain_ref[...]).astype(BF16)
    chosen, first = slots_of(ids_ref[...], capacity, group)
    disp[...] = dot(chosen.astype(BF16), normed).astype(BF16).reshape(disp.shape)

    for copy in small[3:]:
        copy.wait()
    lg[...] = jnp.zeros_like(lg)
    for h in range(heads):
        for b in range(blocks):
            i = h * blocks + b
            lg[i : i + 1, :] = logs_ref[h : h + 1, b * BLOCK : (b + 1) * BLOCK]
    upper = jnp.where(
        lax.broadcasted_iota(jnp.int32, (BLOCK, BLOCK), 0)
        <= lax.broadcasted_iota(jnp.int32, (BLOCK, BLOCK), 1),
        1.0,
        0.0,
    ).astype(BF16)
    la, lb, lc = split3(lg[...])
    sums = dot(la, upper) + dot(lb, upper) + dot(lc, upper)
    cum[...] = sums
    lasts = sums[:, BLOCK - 1 : BLOCK]
    bef[...] = jnp.zeros_like(bef)
    dm[...] = jnp.zeros_like(dm)
    for h in range(heads):
        total = jnp.zeros((1, 1), F32)
        for b in range(blocks):
            i = h * blocks + b
            bef[i : i + 1, :] = jnp.exp(jnp.broadcast_to(total, (1, hd)))
            total = total + lasts[i : i + 1]
        dm[h : h + 1, :] = jnp.exp(jnp.broadcast_to(total, (1, hd)))

    pl.semaphore_wait(barrier, E - 1 + L - 1)
    mids = list(range(E - E // 4, E)) + list(range(E // 2, E - E // 4))
    near = list(range(2, E // 2))
    n4 = len(mids) // 4
    waves = [
        [1] + near[:1] + mids[:n4],
        mids[n4 : 2 * n4],
        near[1:],
        mids[2 * n4 :],
    ]
    order = [0] + waves[0] + waves[1] + waves[2] + waves[3]

    held = len(waves[3])

    def send_wave(i):
        for k in waves[i]:
            token(k).start()

    def pass_on(k):
        token(k).wait_recv()
        for v in range(1, chips):
            across(v, k).start()
        beside(0, k).start()

    def hand_over(k):
        for v in range(1, chips):
            across(v, k).wait_recv()
            beside(v, k).start()

    send_wave(0)
    x_v[t, e] = disp[e]
    for v in range(1, chips):
        across(v, 0).start()
    beside(0, 0).start()
    for k in range(1, G):
        decay(k).start()
    drecv[place] = dm[...]

    def tables_of(b):
        cb, sb = cos_b[e * blocks + b], sin_b[e * blocks + b]
        return cos_r[...] * cb - sin_r[...] * sb, sin_r[...] * cb + cos_r[...] * sb

    def rotate(x, cosine, sine):
        front = x[:, :half].astype(F32)
        rest = x[:, half:].astype(F32)
        return jnp.concatenate([front * cosine - rest * sine, rest * cosine + front * sine], axis=1)

    def column(row):
        return jnp.transpose(jnp.broadcast_to(row, (8, BLOCK)))[:, 0:1]

    def rows_of(b):
        return pl.ds(pl.multiple_of(b * BLOCK, BLOCK), BLOCK)

    for h in range(heads):
        load_head(1, k_hbm, k_v, h).wait()
        load_head(2, v_hbm, v_v, h).wait()
        state[...] = jnp.zeros_like(state)

        def update(b):
            j = h * blocks + b
            at = rows_of(b)
            cum_row = cum[pl.ds(j, 1), :]
            last = cum_row[:, BLOCK - 1 : BLOCK]
            k_rot = (rotate(k_v[h, at, :], *tables_of(b)) * hd ** (-0.5)).astype(BF16)
            k_v[h, at, :] = k_rot
            k_decayed = (k_rot.astype(F32) * jnp.exp(last - column(cum_row))).astype(BF16)
            old = state[...]
            states[j] = old
            state[...] = jnp.exp(last) * old + dot(k_decayed, v_v[h, at, :], 0, 0)
            if h == heads - 1:
                for k, step in ((order[1], 1), (order[2], blocks - 1)):

                    @pl.when(b == step)
                    def _():
                        pass_on(k)

        loop(blocks, update, True)
        smsg[h] = state[...].astype(BF16).reshape(smsg.shape[1:])
        for k in range(1, G):
            scatter(h, k).start()
        srecv[h, place] = smsg[h, place]
        if h == 0:
            send_wave(1)
    load_weight(0).start()
    load_weight(1).start()
    for h in range(heads):
        load_head(3, g_hbm, g_v, h).start()
    load_weight(2).start()
    load_weight(3).start()

    def scan(h, carry):
        for p in range(G):
            pout[h, p] = carry.astype(BF16)
            carry = drecv[p, h : h + 1, :] * carry + srecv[h, p].astype(F32)
        for k in range(1, G):
            spread(h, k).start()
        inc[h, place] = pout[h, place]
        return carry

    def arrivals(h):
        if h == 0:
            done(drecv.at[0 : G - 1], d_r)
        done(srecv.at[h, 0 : G - 1], s1_r.at[h])

    def prefix_low(h):
        @pl.when(upper_half == 0)
        def _():
            arrivals(h)
            carry = scan(h, jnp.zeros(srecv.shape[2:], F32))
            tsend[h] = carry.astype(BF16)
            lift(h).start()

    def prefix_high(h):
        @pl.when(upper_half == 1)
        def _():
            arrivals(h)
            lift(h).wait_recv()
            scan(h, trecv[h].astype(F32))

    def within(j):
        h, b = j // blocks, j % blocks
        for hh in range(heads):

            @pl.when(j == hh * blocks)
            def _():
                load_head(0, q_hbm, q_v, hh).wait()

        at = rows_of(b)
        cum_row = cum[pl.ds(j, 1), :]
        cum_col = column(cum_row)
        q_rot = rotate(q_v[h, at, :], *tables_of(b)).astype(BF16)
        k_rot = k_v[h, at, :]
        value = v_v[h, at, :]
        q_v[h, at, :] = (q_rot.astype(F32) * jnp.exp(cum_col)).astype(BF16)
        step = BLOCK // 2
        for i in range(2):
            r0, reach = i * step, (i + 1) * step
            scores = dot(q_rot[r0 : r0 + step], k_rot[:reach], 1, 1)
            causal = (
                lax.broadcasted_iota(jnp.int32, (step, reach), 0) + r0
                >= lax.broadcasted_iota(jnp.int32, (step, reach), 1)
            )
            gap = cum_col[r0 : r0 + step] - cum_row[:, :reach]
            mask = jnp.exp(jnp.where(causal, gap, -1e30))
            weights = (scores * mask).astype(BF16)
            local[j, r0 : r0 + step, :] = dot(weights, value[:reach])

        for i, k in enumerate(order[3:-held]):

            @pl.when(j == min(1 + 2 * i + i // 2, steps - 1))
            def _():
                pass_on(k)

        for i, k in enumerate(order[:2]):

            @pl.when(j == steps // 2 + min(2 * i, steps // 2 - 1))
            def _():
                hand_over(k)

        for hh in range(heads):
            if high_step(hh) < steps:

                @pl.when(j == high_step(hh))
                def _():
                    prefix_high(hh)

            @pl.when(j == low_step(hh))
            def _():
                prefix_low(hh)
                if hh == 0:
                    send_wave(2)
                if hh == heads - 1:
                    send_wave(3)

    def low_step(h):
        return min(max(0, 3 - 3 * (heads - 1 - h)), steps - 1)

    def high_step(h):
        return low_step(h) + 4

    loop(steps, within)
    for h in range(heads):
        if high_step(h) >= steps:
            prefix_high(h)

    def finish(h):
        done(inc.at[h, 0 : G - 1], s2_r.at[h])
        load_head(3, g_hbm, g_v, h).wait()
        incoming = inc[h].astype(F32).reshape(hd, hd)
        gain = rgain_ref[:, h * hd : (h + 1) * hd]

        def piece(n):
            i = lax.rem(n + 2, L)
            d = lane_ahead(i)
            j = h * blocks + d * R // BLOCK
            at = pl.ds(pl.multiple_of(d * R, R), R)
            inner = pl.ds(pl.multiple_of(lax.rem(d * R, BLOCK), R), R)
            start = bef[pl.ds(j, 1), :] * incoming + states[j]
            retained = local[j, inner, :] + dot(q_v[h, at, :], start.astype(BF16))
            scale = lax.rsqrt(jnp.mean(retained * retained, axis=-1, keepdims=True) + norm_eps)
            gate = g_v[h, at, :].astype(F32)
            gate = gate / (1.0 + jnp.exp(-gate))
            out = (gate * retained * scale * gain).astype(BF16)
            g_v[h, at, :] = out

            @pl.when((i != 0) if h < heads - 1 else ((i != 0) & (i != L - 1)))
            def _():
                head_copy(h, i).start()

            @pl.when(i == 0)
            def _():
                heads_v[:, pl.ds(pl.multiple_of(t * width + h * hd, hd), hd)] = out

        loop(L, piece)

    for k in order[-held:]:
        pass_on(k)
    for h in range(heads):
        finish(h)
        if h == 0:
            for k in order[2:5]:
                hand_over(k)
    for k in order[5:]:
        hand_over(k)

    done(x_v.at[0:chips], gc_r)
    load_weight(0).wait()
    load_weight(1).wait()
    hidden_width = hid.shape[1]
    tile = 256 if hidden_width % 256 == 0 else 128

    def up(n):
        at = pl.ds(pl.multiple_of(n * tile, tile), tile)
        x = x_v[...].reshape(L * group, D)
        both = dot(x, jnp.concatenate([wg_v[:, at], wu_v[:, at]], axis=1))
        gate, rise = both[:, :tile], both[:, tile:]
        hid[:, at] = (gate / (1.0 + jnp.exp(-gate)) * rise).astype(BF16)

    loop(hidden_width // tile, up, True)

    load_weight(2).wait()

    def share(n):
        done(rbuf.at[n], c2_r.at[n])
        for v in range(1, chips):
            yy = chip_ahead(v)
            total = ybuf[n, 2 * yy + c].astype(F32) + rbuf[n, yy].astype(F32)
            ysend[n, v - 1] = total.astype(BF16)
            chip_sum(n, v).start()

    def down(n):
        at = pl.ds(pl.multiple_of(n * COLS, COLS), COLS)
        ybuf[n] = dot(hid[...], wd_v[:, at]).astype(BF16).reshape(ybuf.shape[1:])
        for yy in range(chips):
            core_sum(n, yy).start()

        @pl.when(n > 0)
        def _():
            share(n - 1)

    loop(NT, down)
    share(NT - 1)
    last_copy().start()

    load_weight(3).wait()
    done(heads_v.at[:, 0 : (heads * (L - 1) - 1) * hd], h_r.at[0])
    heads_v[:, last_rows] = jnp.zeros_like(hlast)

    def parts(n):
        for i in range(2):
            at = (2 * n + i) * R
            rows_at = pl.ds(pl.multiple_of(lax.rem(at, BLOCK), R), R)
            yield at // BLOCK, rows_at, slice(i * hd, (i + 1) * hd)

    def project(n):
        at = pl.ds(pl.multiple_of(n * COLS, COLS), COLS)
        sums = dot(heads_v[...], wo_v[:, at])
        for plane, rows_at, cols in parts(n):
            local[plane, rows_at, :] = sums[:, cols]
        total = ybuf[n, t].astype(F32) + rbuf[n, y].astype(F32)
        done(yrecv.at[n], y2_r.at[n])
        for v in range(1, chips):
            total = total + yrecv[n, v - 1].astype(F32)
        fin[n] = total.astype(BF16).reshape(fin.shape[1:])
        for k in range(1, E):
            back(n, k).start()
        ret[n, e] = fin[n, e]

    loop(NT, project)

    weight = chosen * jnp.where(first, rw_ref[0:1, :], rw_ref[1:2, :])
    terms = split3(weight)
    for n in range(NT):
        done(ret.at[n, 0 : E - 1], r_r.at[n])
        got = ret[n].reshape(group, COLS)
        total = dot(terms[0], got, 0, 0) + dot(terms[1], got, 0, 0) + dot(terms[2], got, 0, 0)
        omoe[:, n * COLS : (n + 1) * COLS] = total.astype(BF16)

    last_copy().wait_recv()

    def project_last(n):
        at = pl.ds(pl.multiple_of(n * COLS, COLS), COLS)
        sums = dot(hlast[...], wo_v[last_rows, at])
        for plane, rows_at, cols in parts(n):
            to = pl.ds(pl.multiple_of(n * COLS + cols.start, hd), hd)
            obuf[:, to] = (local[plane, rows_at, :] + sums[:, cols]).astype(BF16)

    loop(NT, project_last, True)

    done(x_v.at[0, 0 : E - 1], a_s)
    done(x_v.at[0 : chips - 1], gy_s)
    done(x_v.at[0:chips], gc_s)
    done(drecv.at[0 : G - 1], d_s)

    @pl.when(upper_half == 0)
    def _():
        done(tsend, t_s)

    for h in range(heads):
        done(smsg.at[h, 0 : G - 1], s1_s.at[h])
        done(pout.at[h, 0 : G - 1], s2_s.at[h])
        done(heads_v.at[:, 0 : (L - 1) * hd], h_s.at[h])
    done(rbuf, c2_s)
    done(ysend, y2_s)
    for n in range(NT):
        done(fin.at[n, 0 : E - 1], r_s.at[n])


def on_device(
    mix_query, mix_key, mix_value, mix_gate, log_decay, ret_gain, w_out,
    moe_in, route_ids, route_weights, moe_gain, w_gate, w_up, w_down,
):
    E = lax.axis_size("ep")
    L = lax.axis_size("tp")
    chips = L // 2
    rows, width = mix_query.shape
    heads = width // HEAD_DIM
    blocks = rows // BLOCK
    steps = heads * blocks
    half = HEAD_DIM // 2
    tokens, D = moe_in.shape
    capacity = 4 * tokens // E
    group = E * capacity
    hidden = w_gate.shape[2]
    NT = D // COLS
    R = rows // L
    G = E // 2
    part = HEAD_DIM // G
    inverse = 10000.0 ** (-(np.arange(half) * 2.0) / HEAD_DIM)
    fine = np.arange(BLOCK)[:, None] * inverse[None, :]
    coarse = (np.arange(E * blocks) * BLOCK)[:, None, None] * inverse[None, None, :]
    tables = [np.asarray(f(x), np.float32) for x in (fine, coarse) for f in (np.cos, np.sin)]
    hbm = pl.BlockSpec(memory_space=pl.ANY)
    pad = -(-steps // 8) * 8
    V = pltpu.VMEM
    S = pltpu.SemaphoreType.DMA
    return pl.pallas_call(
        layer_kernel,
        in_specs=[hbm] * 18,
        out_specs=[pl.BlockSpec(memory_space=pltpu.VMEM)] * 2,
        out_shape=[
            pltpu.VMEM((R, D), BF16),
            pltpu.VMEM((tokens, D), BF16),
        ],
        scratch_shapes=[
            V((tokens, D), BF16), V((2, tokens), jnp.int32), V((2, tokens), F32),
            V((1, D), F32), V((1, width), F32), V((heads, rows), F32),
            V((BLOCK, half), F32), V((BLOCK, half), F32),
            V((E * blocks, 1, half), F32), V((E * blocks, 1, half), F32),
            V((heads, rows, HEAD_DIM), BF16), V((heads, rows, HEAD_DIM), BF16),
            V((heads, rows, HEAD_DIM), BF16), V((heads, rows, HEAD_DIM), BF16),
            V((D, hidden), BF16), V((D, hidden), BF16), V((hidden, D), BF16), V(w_out.shape, BF16),
            V((E, capacity, D), BF16), V((L, E, capacity, D), BF16), V((L * group, hidden), BF16),
            V((NT, L, group, COLS), BF16), V((NT, chips, group, COLS), BF16),
            V((NT, chips - 1, group, COLS), BF16), V((NT, chips - 1, group, COLS), BF16),
            V((NT, E, capacity, COLS), BF16), V((NT, E, capacity, COLS), BF16),
            V((pad, BLOCK), F32), V((pad, BLOCK), F32), V((pad, HEAD_DIM), F32),
            V((steps, BLOCK, HEAD_DIM), F32), V((HEAD_DIM, HEAD_DIM), F32),
            V((steps, HEAD_DIM, HEAD_DIM), F32),
            V((8, HEAD_DIM), F32), V((G, 8, HEAD_DIM), F32),
            V((heads, G, part, HEAD_DIM), BF16), V((heads, G, part, HEAD_DIM), BF16),
            V((heads, part, HEAD_DIM), BF16), V((heads, part, HEAD_DIM), BF16),
            V((heads, G, part, HEAD_DIM), BF16), V((heads, G, part, HEAD_DIM), BF16),
            V((R, D), BF16), V((R, HEAD_DIM), BF16),
            S((10,)), S((4, heads)), S((4,)), S(()), S((E,)),
            S(()), S((chips - 1, E)), S(()), S(()),
            S(()), S(()), S((heads,)), S((heads,)), S(()), S((heads,)), S((heads,)), S((heads,)),
            S((heads,)), S((2,)), S(()), S((NT,)), S(()), S((NT,)), S((NT,)), S((NT,)),
        ],
        compiler_params=pltpu.CompilerParams(
            collective_id=0, has_side_effects=True, vmem_limit_bytes=VMEM_LIMIT
        ),
        name="layer",
    )(
        moe_in, route_ids.T, route_weights.T, moe_gain.reshape(1, -1), ret_gain.reshape(1, -1),
        log_decay.T, *tables,
        mix_query, mix_key, mix_value, mix_gate, w_gate, w_up, w_down, w_out,
    )


def solution(mesh):
    in_specs = (
        P("ep", "tp"),
        P("ep", "tp"),
        P("ep", "tp"),
        P("ep", "tp"),
        P("ep", "tp"),
        P("tp"),
        P(),
        P(("ep", "tp"), None),
        P(("ep", "tp"), None),
        P(("ep", "tp"), None),
        P(),
        P("ep", None, "tp"),
        P("ep", None, "tp"),
        P("ep", "tp", None),
    )
    out_specs = (P(("ep", "tp"), None), P(("ep", "tp"), None))
    return jax.shard_map(
        lambda *args: tuple(on_device(*args)), mesh=mesh, in_specs=in_specs, out_specs=out_specs,
        check_vma=False,
    )
```
